32 devices in a mesh: grp: 2 (over y), sp: 4 (over z), dp: 4 (over x, core).
Axes of the slice: x: 2, y: 2, z: 4, core: 2. Of those that a mesh axis runs over, the one named last changes fastest.
Arguments:
- gate_input: bfloat16 [8, 1536, 2048], P(('grp', 'dp'), 'sp'), parts along dimension 0, may hold values from -6 to 6
- value_input: bfloat16 [8, 1536, 2048], P(('grp', 'dp'), 'sp'), parts along dimension 0, may hold values from -6 to 6
- norm_gain: bfloat16 [2048], replicated, may hold values from 0.099609375 to 1.8984375
- norm_bias: bfloat16 [2048], replicated, may hold values from -2.5 to 2.5
- mix_weight: bfloat16 [16, 1024, 1024], P('sp', 'dp'), may hold values from -0.1875 to 0.1875
- mix_bias: bfloat16 [16, 1024], P('sp'), may hold values from 0.099609375 to 1.8984375
Outputs:
- gated: bfloat16 [8, 1536, 2048], P(('grp', 'dp'), 'sp'), parts along dimension 0
The draws below stay inside these ranges and needn't reach their ends.
There are 2 independent parts, one for each index of `grp`. The reference program is written for one: setup_inputs(seed, part) draws one part's arguments, and reference() takes and returns one part's arrays. A program takes and returns all parts, laid end to end along the dimension named above; an argument that names none is the same for every part. Nothing has to cross between parts.
All inputs are finite; a program needn't handle non-finite values.
Results may differ from the reference program's by a relative error of at most 0.0053.
Values may be sent and summed in bfloat16 or wider, within the bound.
A program may use at most 64 MiB of HBM per device.

```python
import jax
import jax.numpy as jnp
from jax import lax

GD = 128
G = 16
GW = 2048
BLK = 1024
LEN = 1536
SEQS = 4


def level_of(rng, dims, cuts, low, top_value):
    gain = 1.0
    for position, shards_of in cuts:
        draws = jax.random.uniform(jax.random.fold_in(jax.random.fold_in(rng, 6), position), (shards_of,), jnp.float32, low / len(cuts), top_value / len(cuts))
        gain = gain * jnp.repeat(jnp.exp(draws), dims[position] // shards_of).reshape((-1,) + (1,) * (len(dims) - 1 - position))
    return gain


def gaussian(stream_key, dims, deviation, limit, pieces=(), held_as=jnp.bfloat16):
    values = deviation * jax.random.normal(stream_key, dims, jnp.float32)
    if pieces:
        values = values * level_of(stream_key, dims, pieces, -0.22, 0.18)
    return jnp.clip(values, -limit, limit).astype(held_as)


def setup_inputs(seed: int = 0, part: int = 0) -> dict:
    key_of = jax.random.split(jax.random.key(seed), 7)
    part_keys = jax.random.split(jax.random.fold_in(key_of[6], part), 7)
    gate_input = gaussian(part_keys[0], (SEQS, LEN, GW), 1.0, 6.0, ((0, 4), (1, 4)))
    value_input = gaussian(part_keys[1], (SEQS, LEN, GW), 1.0, 6.0, ((0, 4), (1, 4)))
    norm_gain = jnp.clip(1.0 + 0.18 * jax.random.normal(key_of[2], (GW,), jnp.float32), 0.099609375, 1.8984375).astype(jnp.bfloat16)
    norm_bias = gaussian(key_of[3], (GW,), 0.5, 2.5)
    mix_weight = gaussian(key_of[4], (G, BLK, BLK), BLK ** -0.5, 0.1875, ((0, 4), (1, 4)))
    mix_bias = jnp.clip(1.0 + 0.18 * jax.random.normal(key_of[5], (G, BLK), jnp.float32), 0.099609375, 1.8984375).astype(jnp.bfloat16)
    return {"gate_input": gate_input, "value_input": value_input, "norm_gain": norm_gain, "norm_bias": norm_bias, "mix_weight": mix_weight, "mix_bias": mix_bias}


def reference(gate_input, value_input, norm_gain, norm_bias, mix_weight, mix_bias):
    seqs, length, width = value_input.shape
    nblocks = -(-length // BLK)
    act = jax.nn.gelu(value_input.astype(jnp.float32))
    mean = lax.optimization_barrier(jnp.mean(act, axis=-1, keepdims=True))
    var = lax.optimization_barrier(jnp.mean(jnp.square(act - mean), axis=-1, keepdims=True))
    normed = ((act - mean) * lax.rsqrt(var + 1e-06) * norm_gain.astype(jnp.float32) + norm_bias.astype(jnp.float32)).astype(jnp.bfloat16)
    keep = jnp.tril(jnp.ones((BLK, BLK), dtype=bool))
    weight_full = jnp.where(keep[None], mix_weight.astype(jnp.float32), jnp.float32(0.0))
    bias_full = mix_bias.astype(jnp.float32).T[None, :, :, None]

    def mix_sequence(normed_seq):
        padded = jnp.pad(normed_seq, ((0, nblocks * BLK - length), (0, 0)))
        blocks = padded.reshape(nblocks, BLK, G, GD).astype(jnp.float32)
        mixed = jnp.einsum('gts,bsgc->btgc', weight_full, blocks) + bias_full
        return mixed.reshape(nblocks * BLK, width)[:length].astype(jnp.bfloat16)
    mixed = lax.map(mix_sequence, normed)
    mixed = lax.optimization_barrier(mixed)
    gated = jax.nn.gelu(gate_input.astype(jnp.float32)) * mixed.astype(jnp.float32)
    return gated.astype(jnp.bfloat16)
```

```python
import functools

import jax
import jax.numpy as jnp
from jax import lax
from jax.experimental import pallas as pl
from jax.experimental.pallas import tpu as pltpu
from jax.sharding import PartitionSpec as P

GD = 128
BLK = 1024
ROOT_2_PI = 0.7978845608028654


def gelu(x):
    return (0.5 * x) * (1.0 + jnp.tanh(ROOT_2_PI * (x + 0.044715 * (x * x * x))))


def segments(dest, span):
    runs, at = [], dest * span
    while at < (dest + 1) * span:
        stop = min((dest + 1) * span, (at // BLK + 1) * BLK)
        runs.append((at, stop))
        at = stop
    return runs


def kernel(
    ngrp, nsp, ndp, value_hbm, gate_hbm, gain_ref, nbias_ref, w_hbm, mbias_ref, out_ref,
    vbuf, gbuf, ggelu, nsend, ex, rsend, ret, wbuf,
    v_sem, g_sem, w_sem, own_sem, ret_own_sem,
    f_ssem, f_rsem, b_ssem, b_rsem,
    o_ssem, o_rsem, x_ssem, x_rsem, y_ssem, y_rsem, c_ssem, c_rsem,
):
    span, width = vbuf.shape
    cw = width // nsp
    groups = cw // GD
    piece = v_piece(span)
    pieces = span // piece
    nx = ndp // 2
    rows = BLK // ndp
    part = rows // ngrp
    p, z, r = lax.axis_index("grp"), lax.axis_index("sp"), lax.axis_index("dp")
    xi, core = r // 2, r % 2
    mate = r + 1 - 2 * core

    def value_copy(i):
        at = pl.ds(i * piece, piece)
        return pltpu.make_async_copy(value_hbm.at[0, at], vbuf.at[at], v_sem.at[i])

    def own_rows(block, q, count):
        return pl.ds(pl.multiple_of(block * rows + q * part, part), count)

    mine = own_rows(r, 0, rows)
    w_copy = pltpu.make_async_copy(w_hbm, wbuf.at[:, mine], w_sem)
    gate_copy = pltpu.make_async_copy(gate_hbm.at[0], gbuf, g_sem)
    value_copy(0).start()
    w_copy.start()
    for i in range(1, pieces):
        value_copy(i).start()
    gate_copy.start()

    barrier = pltpu.get_barrier_semaphore()
    peers = [{"sp": lax.rem(z + k, nsp)} for k in range(1, nsp)]
    peers += [{"dp": mate}]
    peers += [{"dp": lax.rem(xi + k, nx) * 2 + core} for k in range(1, nx)]
    peers += [{"grp": lax.rem(p + k, ngrp)} for k in range(1, ngrp)]
    for peer in peers:
        pl.semaphore_signal(barrier, inc=1, device_id=peer, device_id_type=pl.DeviceIdType.MESH)
    pl.semaphore_wait(barrier, len(peers))

    def remote(src, dst, ssem, rsem, device):
        return pltpu.make_async_remote_copy(
            src_ref=src, dst_ref=dst, send_sem=ssem, recv_sem=rsem,
            device_id=device, device_id_type=pl.DeviceIdType.MESH,
        )

    upper = z // ((nsp + 1) // 2)

    def peer_at(j):
        return upper * j + (1 - upper) * (nsp - 1 - j)

    def ex_rows(src, i):
        return pl.ds(pl.multiple_of(src * span + i * piece, piece), piece)

    def forward(i, dest, src):
        return remote(
            nsend.at[dest, pl.ds(i * piece, piece)], ex.at[ex_rows(src, i)],
            f_ssem.at[i, dest], f_rsem.at[i, src], {"sp": dest},
        )

    def forward_own(i):
        return pltpu.make_async_copy(
            nsend.at[z, pl.ds(i * piece, piece)], ex.at[ex_rows(z, i)], own_sem.at[i]
        )

    gain = gain_ref[...].astype(jnp.float32)
    nbias = nbias_ref[...].astype(jnp.float32)

    def normalise(i):
        def step(s, carry):
            at = pl.ds(pl.multiple_of(i * piece + s * 16, 16), 16)
            act = gelu(vbuf[at, :].astype(jnp.float32))
            mean = jnp.sum(act, axis=-1, keepdims=True) * (1.0 / width)
            act = act - mean
            var = jnp.sum(act * act, axis=-1, keepdims=True) * (1.0 / width)
            normed = (act * lax.rsqrt(var + 1e-06) * gain + nbias).astype(jnp.bfloat16)
            for t in range(nsp):
                nsend[t, at, :] = normed[:, t * cw:(t + 1) * cw]
            return carry

        lax.fori_loop(0, piece // 16, step, 0, unroll=2)

    def w_own():
        return remote(wbuf.at[:, mine], wbuf.at[:, mine], o_ssem, o_rsem, {"dp": mate})

    def w_own_in():
        at = own_rows(mate, 0, rows)
        return remote(wbuf.at[:, at], wbuf.at[:, at], o_ssem, o_rsem, {"dp": mate})

    def w_x(g, src, dest, slot):
        at = wbuf.at[g, own_rows(src * 2 + core, p, part)]
        return remote(at, at, x_ssem.at[slot, g], x_rsem.at[src, g], {"dp": dest * 2 + core})

    def w_y(g, src, q, slot, dest):
        at = wbuf.at[g, own_rows(src * 2 + core, q, part)]
        return remote(at, at, y_ssem.at[slot, src, g], y_rsem.at[q, src, g], {"grp": dest})

    def w_c(g, src, q, side):
        at = wbuf.at[g, own_rows(src * 2 + side, q, part)]
        return remote(at, at, c_ssem.at[q, src, g], c_rsem.at[q, src, g], {"dp": mate})

    for i in range(pieces):
        value_copy(i).wait()
        normalise(i)
        forward_own(i).start()
        for j in range(nsp):
            dest = peer_at(j)

            @pl.when(dest != z)
            def _(i=i, dest=dest):
                forward(i, dest, z).start()

        if i == 0:
            w_copy.wait()
            for g in range(groups):
                for k in range(1, nx):
                    w_x(g, xi, lax.rem(xi + k, nx), k - 1).start()
            w_own().start()

    def from_y(g):
        for k in range(1, nx):
            src = lax.rem(xi + nx - k, nx)
            for m in range(1, ngrp):
                q = lax.rem(p + ngrp - m, ngrp)
                w_y(g, src, q, m - 1, q).wait_recv()
                w_c(g, src, q, core).start()

    for g in range(groups):
        for k in range(1, nx):
            src = lax.rem(xi + nx - k, nx)
            w_x(g, src, src, k - 1).wait_recv()
            for m in range(1, ngrp):
                w_y(g, src, p, m - 1, lax.rem(p + m, ngrp)).start()
            w_c(g, src, p, core).start()
        if g == 0:
            gate_copy.wait()

            def gate_step(s, carry):
                at = pl.ds(pl.multiple_of(s * 16, 16), 16)
                ggelu[at, :] = gelu(gbuf[at, :].astype(jnp.float32))
                return carry

            lax.fori_loop(0, span // 16, gate_step, 0)
        else:
            from_y(g - 1)
    from_y(groups - 1)
    w_own_in().wait_recv()
    for g in range(groups):
        for k in range(1, nx):
            src = lax.rem(xi + k, nx)
            for q in range(ngrp):
                w_c(g, src, q, 1 - core).wait_recv()

    ready = set()

    def need(src):
        if src in ready:
            return
        ready.add(src)

        @pl.when(z == src)
        def _():
            for i in range(pieces):
                forward_own(i).wait()

        @pl.when(z != src)
        def _():
            for i in range(pieces):
                forward(i, src, src).wait_recv()

    def back(dest, src):
        return remote(
            rsend.at[dest], ret.at[src], b_ssem.at[dest], b_rsem.at[src], {"sp": dest}
        )

    def back_own():
        return pltpu.make_async_copy(rsend.at[z], ret.at[z], ret_own_sem)

    order = []
    for j in range((nsp + 1) // 2):
        order += [j] if j == nsp - 1 - j else [j, nsp - 1 - j]
    for dest in order:
        for at, stop in segments(dest, span):
            base = at // BLK * BLK
            t0, size = at - base, stop - at
            for src in range(base // span, (stop - 1) // span + 1):
                need(src)
            keep = (
                lax.broadcasted_iota(jnp.int32, (size, size), 1)
                <= lax.broadcasted_iota(jnp.int32, (size, size), 0)
            )
            for g in range(groups):
                lanes = slice(g * GD, (g + 1) * GD)
                diag = wbuf[g, t0:t0 + size, t0:t0 + size]
                diag = jnp.where(keep, diag, jnp.zeros_like(diag))
                acc = jnp.dot(diag, ex[at:stop, lanes], preferred_element_type=jnp.float32)
                if t0:
                    acc += jnp.dot(
                        wbuf[g, t0:t0 + size, :t0], ex[base:at, lanes],
                        preferred_element_type=jnp.float32,
                    )
                acc += mbias_ref[t0:t0 + size, g:g + 1]
                rsend[dest, at - dest * span:stop - dest * span, lanes] = acc.astype(jnp.bfloat16)

        @pl.when(z == dest)
        def _():
            back_own().start()

        @pl.when(z != dest)
        def _():
            back(dest, z).start()

    def gate_out(src):
        lanes = pl.ds(pl.multiple_of(src * cw, GD), cw)

        def step(s, carry):
            at = pl.ds(pl.multiple_of(s * 16, 16), 16)
            out_ref[0, at, lanes] = (
                ggelu[at, lanes] * ret[src, at, :].astype(jnp.float32)
            ).astype(jnp.bfloat16)
            return carry

        lax.fori_loop(0, span // 16, step, 0, unroll=2)

    back_own().wait()
    gate_out(z)
    for j in reversed(range(nsp)):
        src = peer_at(j)

        @pl.when(src != z)
        def _(src=src):
            back(src, src).wait_recv()
            gate_out(src)

    for j in range(nsp):
        dest = peer_at(j)

        @pl.when(dest != z)
        def _(dest=dest):
            for i in range(pieces):
                forward(i, dest, z).wait_send()
            back(dest, z).wait_send()

    w_own().wait_send()
    for g in range(groups):
        for k in range(1, nx):
            w_x(g, xi, lax.rem(xi + k, nx), k - 1).wait_send()
            src = lax.rem(xi + k, nx)
            for m in range(1, ngrp):
                w_y(g, src, p, m - 1, lax.rem(p + m, ngrp)).wait_send()
            for q in range(ngrp):
                w_c(g, src, q, core).wait_send()


def v_piece(span):
    return 128 if span % 128 == 0 else span


def body(ngrp, nsp, ndp, gate_input, value_input, norm_gain, norm_bias, mix_weight, mix_bias):
    _, span, width = value_input.shape
    groups = mix_weight.shape[0]
    cw = groups * GD
    pieces = span // v_piece(span)
    nx = ndp // 2
    dma = pltpu.SemaphoreType.DMA
    bf16, f32 = jnp.bfloat16, jnp.float32
    vmem, hbm = pl.BlockSpec(memory_space=pltpu.VMEM), pl.BlockSpec(memory_space=pl.ANY)
    return pl.pallas_call(
        functools.partial(kernel, ngrp, nsp, ndp),
        out_shape=jax.ShapeDtypeStruct(value_input.shape, bf16),
        in_specs=[hbm, hbm, vmem, vmem, hbm, vmem],
        out_specs=vmem,
        scratch_shapes=[
            pltpu.VMEM((span, width), bf16),
            pltpu.VMEM((span, width), bf16),
            pltpu.VMEM((span, width), f32),
            pltpu.VMEM((nsp, span, cw), bf16),
            pltpu.VMEM((nsp * span, cw), bf16),
            pltpu.VMEM((nsp, span, cw), bf16),
            pltpu.VMEM((nsp, span, cw), bf16),
            pltpu.VMEM((groups, BLK, BLK), bf16),
            dma((pieces,)), dma, dma, dma((pieces,)), dma,
            dma((pieces, nsp)), dma((pieces, nsp)), dma((nsp,)), dma((nsp,)),
            dma, dma,
            dma((max(nx - 1, 1), groups)), dma((nx, groups)),
            dma((max(ngrp - 1, 1), nx, groups)), dma((ngrp, nx, groups)),
            dma((ngrp, nx, groups)), dma((ngrp, nx, groups)),
        ],
        compiler_params=pltpu.CompilerParams(
            collective_id=0, has_side_effects=True, vmem_limit_bytes=50 * 1024 * 1024
        ),
    )(
        value_input, gate_input, norm_gain[None], norm_bias[None], mix_weight,
        mix_bias.astype(f32).T,
    )


def solution(mesh):
    placed = (
        P(("grp", "dp"), "sp", None),
        P(("grp", "dp"), "sp", None),
        P(),
        P(),
        P("sp", "dp", None),
        P("sp", None),
    )
    return jax.shard_map(
        functools.partial(body, mesh.shape["grp"], mesh.shape["sp"], mesh.shape["dp"]),
        mesh=mesh, in_specs=placed, out_specs=P(("grp", "dp"), "sp", None), check_vma=False,
    )
```

```python
import functools

import jax
import jax.numpy as jnp
from jax import lax
from jax.experimental import pallas as pl
from jax.experimental.pallas import tpu as pltpu
from jax.sharding import PartitionSpec as P

GD = 128
BLK = 1024
ROOT_2_PI = 0.7978845608028654


def gelu(x):
    return (0.5 * x) * (1.0 + jnp.tanh(ROOT_2_PI * (x + 0.044715 * (x * x * x))))


def guest_rows(ngrp, nsp, ndp, span):
    length, rows = nsp * span, BLK // ndp
    tail = length - BLK
    fits = nsp % 2 == 0 and ndp == 4 and ngrp == 2 and tail == 2 * rows
    return tail if fits and 2 * tail <= length and v_piece(span) == 128 else 0


def kernel(
    ngrp, nsp, ndp, value_hbm, gate_hbm, gain_ref, nbias_ref, w_hbm, mbias_ref, out_ref,
    vbuf, gbuf, ggelu, nsend, ex, rsend, ret, wbuf, wguest,
    v_sem, g_sem, w_sem, own_sem, ret_own_sem,
    f_ssem, f_rsem, b_ssem, b_rsem,
    o_ssem, o_rsem, x_ssem, x_rsem, y_ssem, y_rsem, c_ssem, c_rsem,
    gz_ssem, gz_rsem, gx_ssem, gx_rsem, gy_ssem, gy_rsem, gc_ssem, gc_rsem,
):
    span, width = vbuf.shape
    cw = width // nsp
    groups = cw // GD
    piece = v_piece(span)
    pieces = span // piece
    total = nsp * pieces
    tail = guest_rows(ngrp, nsp, ndp, span)
    half = (nsp + 1) // 2
    nx = ndp // 2
    rows = BLK // ndp
    part = rows // ngrp
    p, z, r = lax.axis_index("grp"), lax.axis_index("sp"), lax.axis_index("dp")
    xi, core = r // 2, r % 2
    mate = r + 1 - 2 * core
    upper = z // half

    def value_copy(i):
        at = pl.ds(i * piece, piece)
        return pltpu.make_async_copy(value_hbm.at[0, at], vbuf.at[at], v_sem.at[i])

    def own_rows(block, q, count):
        return pl.ds(pl.multiple_of(block * rows + q * part, part), count)

    mine = own_rows(r, 0, rows)
    w_copy = pltpu.make_async_copy(w_hbm, wbuf.at[:, mine], w_sem)
    gate_copy = pltpu.make_async_copy(gate_hbm.at[0], gbuf, g_sem)
    value_copy(0).start()
    w_copy.start()
    for i in range(1, pieces):
        value_copy(i).start()
    gate_copy.start()

    barrier = pltpu.get_barrier_semaphore()
    peers = [{"sp": lax.rem(z + k, nsp)} for k in range(1, nsp)]
    peers += [{"dp": mate}]
    peers += [{"dp": lax.rem(xi + k, nx) * 2 + core} for k in range(1, nx)]
    peers += [{"grp": lax.rem(p + k, ngrp)} for k in range(1, ngrp)]
    for peer in peers:
        pl.semaphore_signal(barrier, inc=1, device_id=peer, device_id_type=pl.DeviceIdType.MESH)
    pl.semaphore_wait(barrier, len(peers))

    def remote(src, dst, ssem, rsem, device):
        return pltpu.make_async_remote_copy(
            src_ref=src, dst_ref=dst, send_sem=ssem, recv_sem=rsem,
            device_id=device, device_id_type=pl.DeviceIdType.MESH,
        )

    def peer_at(j):
        return upper * j + (1 - upper) * (nsp - 1 - j)

    def kind_of(gp, c):
        if not tail:
            return 0
        return (gp * piece // BLK) * (1 - c // half)

    def at_piece(gp, kind):
        return pl.ds(pl.multiple_of(gp * piece + kind * tail, piece), piece)

    def forward(i, c, src, kind):
        return remote(
            nsend.at[c, pl.ds(i * piece, piece)], ex.at[at_piece(src * pieces + i, kind)],
            f_ssem.at[i, c], f_rsem.at[kind, i, src], {"sp": c + half * kind},
        )

    def forward_own(i, c, kind):
        return pltpu.make_async_copy(
            nsend.at[c, pl.ds(i * piece, piece)], ex.at[at_piece(z * pieces + i, kind)],
            own_sem.at[kind, i],
        )

    def each_chunk(i, remote_step, own_step):
        for j in range(nsp):
            c = peer_at(j)
            kind = kind_of(z * pieces + i, c)

            @pl.when(c + half * kind != z)
            def _(c=c, kind=kind):
                remote_step(i, c, kind)

            if own_step is not None:
                @pl.when(c + half * kind == z)
                def _(c=c, kind=kind):
                    own_step(i, c, kind)

    gain = gain_ref[...].astype(jnp.float32)
    nbias = nbias_ref[...].astype(jnp.float32)

    def normalise(i):
        def step(s, carry):
            at = pl.ds(pl.multiple_of(i * piece + s * 16, 16), 16)
            act = gelu(vbuf[at, :].astype(jnp.float32))
            mean = jnp.sum(act, axis=-1, keepdims=True) * (1.0 / width)
            act = act - mean
            var = jnp.sum(act * act, axis=-1, keepdims=True) * (1.0 / width)
            normed = (act * lax.rsqrt(var + 1e-06) * gain + nbias).astype(jnp.bfloat16)
            for t in range(nsp):
                nsend[t, at, :] = normed[:, t * cw:(t + 1) * cw]
            return carry

        lax.fori_loop(0, piece // 16, step, 0, unroll=2)

    hc = BLK // 2

    def halves(src, action):
        action(0)

        @pl.when(src >= nx // 2)
        def _():
            action(1)

    def w_own(h):
        at = wbuf.at[:, mine, pl.ds(h * hc, hc)]
        return remote(at, at, o_ssem.at[h], o_rsem.at[h], {"dp": mate})

    def w_own_in(h):
        at = wbuf.at[:, own_rows(mate, 0, rows), pl.ds(h * hc, hc)]
        return remote(at, at, o_ssem.at[h], o_rsem.at[h], {"dp": mate})

    def w_x(g, src, dest, slot, h):
        at = wbuf.at[g, own_rows(src * 2 + core, p, part), pl.ds(h * hc, hc)]
        return remote(
            at, at, x_ssem.at[slot, g, h], x_rsem.at[src, g, h], {"dp": dest * 2 + core}
        )

    def w_y(g, src, q, slot, dest, h):
        at = wbuf.at[g, own_rows(src * 2 + core, q, part), pl.ds(h * hc, hc)]
        return remote(at, at, y_ssem.at[slot, src, g, h], y_rsem.at[q, src, g, h], {"grp": dest})

    def w_c(g, src, q, side, h):
        at = wbuf.at[g, own_rows(src * 2 + side, q, part), pl.ds(h * hc, hc)]
        return remote(at, at, c_ssem.at[q, src, g, h], c_rsem.at[q, src, g, h], {"dp": mate})

    def guest_at(g, q, side):
        return wguest.at[g, own_rows(side, q, part)]

    def gz(g, dest):
        at = wbuf.at[g, own_rows(core, p, part), pl.ds(0, tail)]
        return remote(at, guest_at(g, p, core), gz_ssem.at[g], gz_rsem.at[g], {"sp": dest})

    def gx(g):
        at = guest_at(g, p, core)
        return remote(at, at, gx_ssem.at[g], gx_rsem.at[g], {"dp": (1 - xi) * 2 + core})

    def gy(g, q):
        at = guest_at(g, q, core)
        return remote(at, at, gy_ssem.at[g], gy_rsem.at[g], {"grp": 1 - p})

    def gc(g, q, side):
        at = guest_at(g, q, side)
        return remote(at, at, gc_ssem.at[q, g], gc_rsem.at[q, g], {"dp": mate})

    odd = [g for g in range(groups) if g % 2]
    even = [g for g in range(groups) if not g % 2]

    def from_x(g):
        for k in range(1, nx):
            src = lax.rem(xi + nx - k, nx)

            def pass_on(h, src=src, k=k):
                w_x(g, src, src, k - 1, h).wait_recv()
                for m in range(1, ngrp):
                    w_y(g, src, p, m - 1, lax.rem(p + m, ngrp), h).start()
                w_c(g, src, p, core, h).start()

            halves(src, pass_on)
        if tail and g % 2:
            @pl.when((upper == 0) & (xi == 1))
            def _():
                gz(g, z + half).start()

    def from_y(g):
        for k in range(1, nx):
            src = lax.rem(xi + nx - k, nx)
            for m in range(1, ngrp):
                q = lax.rem(p + ngrp - m, ngrp)

                def pass_on(h, src=src, m=m, q=q):
                    w_y(g, src, q, m - 1, q, h).wait_recv()
                    w_c(g, src, q, core, h).start()

                halves(src, pass_on)

    for i in range(pieces):
        if i == pieces - 1:
            for g in odd:
                from_x(g)
        value_copy(i).wait()
        normalise(i)
        each_chunk(
            i,
            lambda i, c, kind: forward(i, c, z, kind).start(),
            lambda i, c, kind: forward_own(i, c, kind).start(),
        )
        if i == 0:
            w_copy.wait()
            for g in odd + even:
                for k in range(1, nx):
                    halves(xi, lambda h, g=g, k=k: w_x(
                        g, xi, lax.rem(xi + k, nx), k - 1, h).start())
            halves(xi, lambda h: w_own(h).start())
            if tail:
                @pl.when((upper == 0) & (xi == 0))
                def _():
                    for g in even:
                        gz(g, z + half).start()

    gate_copy.wait()

    def gate_step(s, carry):
        at = pl.ds(pl.multiple_of(s * 16, 16), 16)
        ggelu[at, :] = gelu(gbuf[at, :].astype(jnp.float32))
        return carry

    lax.fori_loop(0, span // 16, gate_step, 0)
    for g in odd:
        from_y(g)
    for g in even:
        from_x(g)
    for g in even:
        from_y(g)

    weights_in = set()

    def need_weights(block):
        if block in weights_in:
            return
        weights_in.add(block)
        src, side = block // 2, block % 2

        @pl.when((src == xi) & (side != core))
        def _():
            for h in range(1 + (src >= nx // 2)):
                w_own_in(h).wait_recv()

        @pl.when((src != xi) & (side != core))
        def _():
            for g in range(groups):
                for q in range(ngrp):
                    for h in range(1 + (src >= nx // 2)):
                        w_c(g, src, q, side, h).wait_recv()

    ready = set()

    def need(gp, kind):
        if (gp, kind) in ready:
            return
        ready.add((gp, kind))
        src, i = gp // pieces, gp % pieces

        @pl.when(z == src)
        def _():
            forward_own(i, z - half * kind, kind).wait()

        @pl.when(z != src)
        def _():
            forward(i, z - half * kind, src, kind).wait_recv()

    def back(gp, c, kind, dest):
        at = pl.ds((gp % pieces) * piece, piece)
        return remote(
            rsend.at[at_piece(gp, kind)], ret.at[c, at],
            b_ssem.at[kind, gp], b_rsem.at[c, gp % pieces], {"sp": dest},
        )

    def back_own(gp, c, kind, i):
        return pltpu.make_async_copy(
            rsend.at[at_piece(gp, kind)], ret.at[c, pl.ds(i * piece, piece)],
            ret_own_sem.at[kind, i],
        )

    def mix(gp, kind):
        at = gp * piece
        base = at // BLK * BLK
        t0 = at - base
        for block in range(t0 // rows, (t0 + piece - 1) // rows + 1):
            if not kind:
                need_weights(block)
        for other in range(base // piece, gp + 1):
            need(other, kind)
        weights = wguest if kind else wbuf
        keep = (
            lax.broadcasted_iota(jnp.int32, (piece, piece), 1)
            <= lax.broadcasted_iota(jnp.int32, (piece, piece), 0)
        )
        lo, mid = base + kind * tail, at + kind * tail
        for g in range(groups):
            lanes = slice(g * GD, (g + 1) * GD)
            diag = weights[g, t0:t0 + piece, t0:t0 + piece]
            diag = jnp.where(keep, diag, jnp.zeros_like(diag))
            acc = jnp.dot(diag, ex[mid:mid + piece, lanes], preferred_element_type=jnp.float32)
            if t0:
                acc += jnp.dot(
                    weights[g, t0:t0 + piece, :t0], ex[lo:mid, lanes],
                    preferred_element_type=jnp.float32,
                )
            col = g + groups * kind
            acc += mbias_ref[t0:t0 + piece, col:col + 1]
            rsend[mid:mid + piece, lanes] = acc.astype(jnp.bfloat16)
        dest = gp // pieces

        @pl.when(z == dest)
        def _():
            back_own(gp, z - half * kind, kind, gp % pieces).start()

        @pl.when(z != dest)
        def _():
            back(gp, z - half * kind, kind, dest).start()

    if tail:
        first_late = BLK // piece

        @pl.when(upper == 1)
        def _():
            for gp in range(first_late, total):
                mix(gp, 0)

        late_blocks = sorted(weights_in)
        weights_in.clear()

        @pl.when(upper == 0)
        def _():
            for block in late_blocks:
                need_weights(block)

        mix(0, 0)
        mix(1, 0)

        @pl.when(upper == 1)
        def _():
            pairs = groups // 2
            near = [2 * k + xi for k in range(pairs)]
            far = [2 * k + 1 - xi for k in range(pairs)]
            for g in near:
                gz(g, z).wait_recv()
                gx(g).start()
                gy(g, p).start()
                gc(g, p, core).start()
            for g in far:
                gx(g).wait_recv()
                gy(g, p).start()
                gc(g, p, core).start()
            for g in near + far:
                gy(g, 1 - p).wait_recv()
                gc(g, 1 - p, core).start()

        mix(2, 0)

        @pl.when(upper == 1)
        def _():
            for g in range(groups):
                for q in range(ngrp):
                    gc(g, q, 1 - core).wait_recv()
            for gp in range(first_late, total):
                mix(gp, 1)

        for gp in range(3, first_late):
            mix(gp, 0)
    else:
        for gp in range(total):
            mix(gp, 0)

    def gate_out(i, c):
        lanes = pl.ds(pl.multiple_of(c * cw, GD), cw)

        def step(s, carry):
            at = pl.ds(pl.multiple_of(i * piece + s * 16, 16), 16)
            out_ref[0, at, lanes] = (
                ggelu[at, lanes] * ret[c, at, :].astype(jnp.float32)
            ).astype(jnp.bfloat16)
            return carry

        lax.fori_loop(0, piece // 16, step, 0, unroll=2)

    for i in range(pieces):
        for j in reversed(range(nsp)):
            c = peer_at(j)
            gp = z * pieces + i
            kind = kind_of(gp, c)

            @pl.when(c + half * kind == z)
            def _(gp=gp, c=c, kind=kind, i=i):
                back_own(gp, c, kind, i).wait()

            @pl.when(c + half * kind != z)
            def _(c=c, i=i):
                back(i, c, 0, c).wait_recv()

            gate_out(i, c)

    for i in range(pieces):
        each_chunk(i, lambda i, c, kind: forward(i, c, z, kind).wait_send(), None)

    def back_sent(gp, kind):
        @pl.when(z != gp // pieces)
        def _():
            back(gp, z - half * kind, kind, gp // pieces).wait_send()

    early = BLK // piece if tail else total
    for gp in range(early):
        back_sent(gp, 0)
    if tail:
        @pl.when(upper == 1)
        def _():
            for gp in range(early, total):
                back_sent(gp, 0)
                back_sent(gp, 1)
            for g in range(groups):
                gy(g, p).wait_send()
                for q in range(ngrp):
                    gc(g, q, core).wait_send()
            for k in range(groups // 2):
                gx(2 * k + xi).wait_send()

        @pl.when(upper == 0)
        def _():
            for k in range(groups // 2):
                gz(2 * k + xi, z + half).wait_send()

    halves(xi, lambda h: w_own(h).wait_send())
    for g in range(groups):
        for k in range(1, nx):
            halves(xi, lambda h: w_x(g, xi, lax.rem(xi + k, nx), k - 1, h).wait_send())
            src = lax.rem(xi + k, nx)

            def sent(h):
                for m in range(1, ngrp):
                    w_y(g, src, p, m - 1, lax.rem(p + m, ngrp), h).wait_send()
                for q in range(ngrp):
                    w_c(g, src, q, core, h).wait_send()

            halves(src, sent)


def v_piece(span):
    return 128 if span % 128 == 0 else span


def body(ngrp, nsp, ndp, gate_input, value_input, norm_gain, norm_bias, mix_weight, mix_bias):
    _, span, width = value_input.shape
    groups = mix_weight.shape[0]
    cw = groups * GD
    pieces = span // v_piece(span)
    nx = ndp // 2
    total = nsp * pieces
    tail = guest_rows(ngrp, nsp, ndp, span)
    kinds, guest = (2, tail) if tail else (1, 16)
    bias = mix_bias.astype(jnp.float32)
    if tail:
        half = nsp // 2
        shifted = lax.ppermute(bias, "sp", [(k, k + half) for k in range(half)])
        bias = jnp.concatenate([bias, shifted])
    dma = pltpu.SemaphoreType.DMA
    bf16, f32 = jnp.bfloat16, jnp.float32
    vmem, hbm = pl.BlockSpec(memory_space=pltpu.VMEM), pl.BlockSpec(memory_space=pl.ANY)
    return pl.pallas_call(
        functools.partial(kernel, ngrp, nsp, ndp),
        out_shape=jax.ShapeDtypeStruct(value_input.shape, bf16),
        in_specs=[hbm, hbm, vmem, vmem, hbm, vmem],
        out_specs=vmem,
        scratch_shapes=[
            pltpu.VMEM((span, width), bf16),
            pltpu.VMEM((span, width), bf16),
            pltpu.VMEM((span, width), f32),
            pltpu.VMEM((nsp, span, cw), bf16),
            pltpu.VMEM((nsp * span + tail, cw), bf16),
            pltpu.VMEM((nsp * span + tail, cw), bf16),
            pltpu.VMEM((nsp, span, cw), bf16),
            pltpu.VMEM((groups, BLK, BLK), bf16),
            pltpu.VMEM((groups, guest, guest), bf16),
            dma((pieces,)), dma, dma, dma((kinds, pieces)), dma((kinds, pieces)),
            dma((pieces, nsp)), dma((kinds, pieces, nsp)),
            dma((kinds, total)), dma((nsp, pieces)),
            dma((2,)), dma((2,)),
            dma((max(nx - 1, 1), groups, 2)), dma((nx, groups, 2)),
            dma((max(ngrp - 1, 1), nx, groups, 2)), dma((ngrp, nx, groups, 2)),
            dma((ngrp, nx, groups, 2)), dma((ngrp, nx, groups, 2)),
            dma((groups,)), dma((groups,)), dma((groups,)), dma((groups,)),
            dma((groups,)), dma((groups,)), dma((ngrp, groups)), dma((ngrp, groups)),
        ],
        compiler_params=pltpu.CompilerParams(
            collective_id=0, has_side_effects=True, vmem_limit_bytes=50 * 1024 * 1024
        ),
    )(
        value_input, gate_input, norm_gain[None], norm_bias[None], mix_weight,
        bias.T,
    )


def solution(mesh):
    placed = (
        P(("grp", "dp"), "sp", None),
        P(("grp", "dp"), "sp", None),
        P(),
        P(),
        P("sp", "dp", None),
        P("sp", None),
    )
    return jax.shard_map(
        functools.partial(body, mesh.shape["grp"], mesh.shape["sp"], mesh.shape["dp"]),
        mesh=mesh, in_specs=placed, out_specs=P(("grp", "dp"), "sp", None), check_vma=False,
    )
```

```python
import functools

import jax
import jax.numpy as jnp
from jax import lax
from jax.experimental import pallas as pl
from jax.experimental.pallas import tpu as pltpu
from jax.sharding import PartitionSpec as P

GD = 128
BLK = 1024
ROOT_2_PI = 0.7978845608028654


def gelu(x):
    return (0.5 * x) * (1.0 + jnp.tanh(ROOT_2_PI * (x + 0.044715 * (x * x * x))))


def guest_rows(ngrp, nsp, ndp, span):
    length, rows = nsp * span, BLK // ndp
    tail = length - BLK
    fits = nsp % 2 == 0 and ndp == 4 and ngrp == 2 and tail == 2 * rows
    return tail if fits and 2 * tail <= length and v_piece(span) == 128 else 0


def kernel(
    ngrp, nsp, ndp, value_hbm, gate_hbm, gain_ref, nbias_ref, w_hbm, mbias_ref, out_ref,
    vbuf, gbuf, ggelu, nsend, ex, rsend, ret, wbuf, wguest, gbias, bcol,
    v_sem, g_sem, w_sem, own_sem, ret_own_sem,
    f_ssem, f_rsem, b_ssem, b_rsem,
    o_ssem, o_rsem, x_ssem, x_rsem, y_ssem, y_rsem, c_ssem, c_rsem,
    gz_ssem, gz_rsem, gx_ssem, gx_rsem, gy_ssem, gy_rsem, gc_ssem, gc_rsem, gb_ssem, gb_rsem,
):
    span, width = vbuf.shape
    cw = width // nsp
    groups = cw // GD
    piece = v_piece(span)
    pieces = span // piece
    total = nsp * pieces
    tail = guest_rows(ngrp, nsp, ndp, span)
    half = (nsp + 1) // 2
    nx = ndp // 2
    rows = BLK // ndp
    part = rows // ngrp
    p, z, r = lax.axis_index("grp"), lax.axis_index("sp"), lax.axis_index("dp")
    xi, core = r // 2, r % 2
    mate = r + 1 - 2 * core
    upper = z // half

    def value_copy(i):
        at = pl.ds(i * piece, piece)
        return pltpu.make_async_copy(value_hbm.at[0, at], vbuf.at[at], v_sem.at[i])

    def own_rows(block, q, count):
        return pl.ds(pl.multiple_of(block * rows + q * part, part), count)

    mine = own_rows(r, 0, rows)
    w_copy = pltpu.make_async_copy(w_hbm, wbuf.at[:, mine], w_sem)
    gate_copy = pltpu.make_async_copy(gate_hbm.at[0], gbuf, g_sem)
    w_copy.start()
    value_copy(0).start()
    for i in range(1, pieces):
        value_copy(i).start()
    gate_copy.start()

    barrier = pltpu.get_barrier_semaphore()
    peers = [{"sp": lax.rem(z + k, nsp)} for k in range(1, nsp)]
    peers += [{"dp": mate}]
    peers += [{"dp": lax.rem(xi + k, nx) * 2 + core} for k in range(1, nx)]
    peers += [{"grp": lax.rem(p + k, ngrp)} for k in range(1, ngrp)]
    for peer in peers:
        pl.semaphore_signal(barrier, inc=1, device_id=peer, device_id_type=pl.DeviceIdType.MESH)
    pl.semaphore_wait(barrier, len(peers))

    def remote(src, dst, ssem, rsem, device):
        return pltpu.make_async_remote_copy(
            src_ref=src, dst_ref=dst, send_sem=ssem, recv_sem=rsem,
            device_id=device, device_id_type=pl.DeviceIdType.MESH,
        )

    def peer_at(j):
        return upper * j + (1 - upper) * (nsp - 1 - j)

    def kind_of(gp, c):
        if not tail:
            return 0
        return (gp * piece // BLK) * (1 - c // half)

    def at_piece(gp, kind):
        return pl.ds(pl.multiple_of(gp * piece + kind * tail, piece), piece)

    def forward(i, c, src, kind):
        return remote(
            nsend.at[c, pl.ds(i * piece, piece)], ex.at[at_piece(src * pieces + i, kind)],
            f_ssem.at[i, c], f_rsem.at[kind, i, src], {"sp": c + half * kind},
        )

    def forward_own(i, c, kind):
        return pltpu.make_async_copy(
            nsend.at[c, pl.ds(i * piece, piece)], ex.at[at_piece(z * pieces + i, kind)],
            own_sem.at[kind, i],
        )

    def each_chunk(i, remote_step, own_step):
        for j in range(nsp):
            c = peer_at(j)
            kind = kind_of(z * pieces + i, c)

            @pl.when(c + half * kind != z)
            def _(c=c, kind=kind):
                remote_step(i, c, kind)

            if own_step is not None:
                @pl.when(c + half * kind == z)
                def _(c=c, kind=kind):
                    own_step(i, c, kind)

    gain = gain_ref[...].astype(jnp.float32)
    nbias = nbias_ref[...].astype(jnp.float32)

    def normalise(i):
        def step(s, carry):
            at = pl.ds(pl.multiple_of(i * piece + s * 16, 16), 16)
            act = gelu(vbuf[at, :].astype(jnp.float32))
            mean = jnp.sum(act, axis=-1, keepdims=True) * (1.0 / width)
            act = act - mean
            var = jnp.sum(act * act, axis=-1, keepdims=True) * (1.0 / width)
            normed = (act * lax.rsqrt(var + 1e-06) * gain + nbias).astype(jnp.bfloat16)
            for t in range(nsp):
                nsend[t, at, :] = normed[:, t * cw:(t + 1) * cw]
            return carry

        lax.fori_loop(0, piece // 16, step, 0, unroll=2)

    hc = BLK // 2

    def halves(src, action):
        action(0)

        @pl.when(src >= nx // 2)
        def _():
            action(1)

    def w_own(h):
        at = wbuf.at[:, mine, pl.ds(h * hc, hc)]
        return remote(at, at, o_ssem.at[h], o_rsem.at[h], {"dp": mate})

    def w_own_in(h):
        at = wbuf.at[:, own_rows(mate, 0, rows), pl.ds(h * hc, hc)]
        return remote(at, at, o_ssem.at[h], o_rsem.at[h], {"dp": mate})

    def w_x(g, src, dest, slot, h):
        at = wbuf.at[g, own_rows(src * 2 + core, p, part), pl.ds(h * hc, hc)]
        return remote(
            at, at, x_ssem.at[slot, g, h], x_rsem.at[src, g, h], {"dp": dest * 2 + core}
        )

    def w_y(g, src, q, slot, dest, h):
        at = wbuf.at[g, own_rows(src * 2 + core, q, part), pl.ds(h * hc, hc)]
        return remote(at, at, y_ssem.at[slot, src, g, h], y_rsem.at[q, src, g, h], {"grp": dest})

    def w_c(g, src, q, side, h):
        at = wbuf.at[g, own_rows(src * 2 + side, q, part), pl.ds(h * hc, hc)]
        return remote(at, at, c_ssem.at[q, src, g, h], c_rsem.at[q, src, g, h], {"dp": mate})

    def guest_at(g, q, side):
        return wguest.at[g, own_rows(side, q, part)]

    def gz(g, dest):
        at = wbuf.at[g, own_rows(core, p, part), pl.ds(0, tail)]
        return remote(at, guest_at(g, p, core), gz_ssem.at[g], gz_rsem.at[g], {"sp": dest})

    def gx(g):
        at = guest_at(g, p, core)
        return remote(at, at, gx_ssem.at[g], gx_rsem.at[g], {"dp": (1 - xi) * 2 + core})

    def gy(g, q):
        at = guest_at(g, q, core)
        return remote(at, at, gy_ssem.at[g], gy_rsem.at[g], {"grp": 1 - p})

    def gc(g, q, side):
        at = guest_at(g, q, side)
        return remote(at, at, gc_ssem.at[q, g], gc_rsem.at[q, g], {"dp": mate})

    odd = [g for g in range(groups) if g % 2]
    even = [g for g in range(groups) if not g % 2]

    def from_x(g):
        for k in range(1, nx):
            src = lax.rem(xi + nx - k, nx)

            def pass_on(h, src=src, k=k):
                w_x(g, src, src, k - 1, h).wait_recv()
                for m in range(1, ngrp):
                    w_y(g, src, p, m - 1, lax.rem(p + m, ngrp), h).start()
                w_c(g, src, p, core, h).start()

            halves(src, pass_on)
        if tail and g % 2:
            @pl.when((upper == 0) & (xi == 1))
            def _():
                gz(g, z + half).start()

    def from_y(g):
        for k in range(1, nx):
            src = lax.rem(xi + nx - k, nx)
            for m in range(1, ngrp):
                q = lax.rem(p + ngrp - m, ngrp)

                def pass_on(h, src=src, m=m, q=q):
                    w_y(g, src, q, m - 1, q, h).wait_recv()
                    w_c(g, src, q, core, h).start()

                halves(src, pass_on)

    def bias_up(dest):
        return remote(mbias_ref, gbias, gb_ssem, gb_rsem, {"sp": dest})

    if tail:
        @pl.when(upper == 0)
        def _():
            bias_up(z + half).start()

    w_copy.wait()
    for g in odd + even:
        for k in range(1, nx):
            halves(xi, lambda h, g=g, k=k: w_x(
                g, xi, lax.rem(xi + k, nx), k - 1, h).start())
    halves(xi, lambda h: w_own(h).start())
    if tail:
        @pl.when((upper == 0) & (xi == 0))
        def _():
            for g in even:
                gz(g, z + half).start()

    for i in range(pieces):
        if i == pieces - 1:
            for g in odd:
                from_x(g)
        value_copy(i).wait()
        normalise(i)
        each_chunk(
            i,
            lambda i, c, kind: forward(i, c, z, kind).start(),
            lambda i, c, kind: forward_own(i, c, kind).start(),
        )

    bcol[0] = mbias_ref[...].T
    gate_copy.wait()

    def gate_step(s, carry):
        at = pl.ds(pl.multiple_of(s * 16, 16), 16)
        ggelu[at, :] = gelu(gbuf[at, :].astype(jnp.float32))
        return carry

    lax.fori_loop(0, span // 16, gate_step, 0)
    for g in odd:
        from_y(g)

    def rest_of_weights():
        for g in even:
            from_x(g)
        for g in even:
            from_y(g)

    if tail:
        @pl.when(xi == 1)
        def _():
            rest_of_weights()
    else:
        rest_of_weights()

    weights_in = set()

    def need_weights(block):
        if block in weights_in:
            return
        weights_in.add(block)
        src, side = block // 2, block % 2

        @pl.when((src == xi) & (side != core))
        def _():
            for h in range(1 + (src >= nx // 2)):
                w_own_in(h).wait_recv()

        @pl.when((src != xi) & (side != core))
        def _():
            for g in range(groups):
                for q in range(ngrp):
                    for h in range(1 + (src >= nx // 2)):
                        w_c(g, src, q, side, h).wait_recv()

    ready = set()

    def need(gp, kind):
        if (gp, kind) in ready:
            return
        ready.add((gp, kind))
        src, i = gp // pieces, gp % pieces

        @pl.when(z == src)
        def _():
            forward_own(i, z - half * kind, kind).wait()

        @pl.when(z != src)
        def _():
            forward(i, z - half * kind, src, kind).wait_recv()

    def back(gp, c, kind, dest):
        at = pl.ds((gp % pieces) * piece, piece)
        return remote(
            rsend.at[at_piece(gp, kind)], ret.at[c, at],
            b_ssem.at[kind, gp], b_rsem.at[c, gp % pieces], {"sp": dest},
        )

    def back_own(gp, c, kind, i):
        return pltpu.make_async_copy(
            rsend.at[at_piece(gp, kind)], ret.at[c, pl.ds(i * piece, piece)],
            ret_own_sem.at[kind, i],
        )

    def mix(gp, kind):
        at = gp * piece
        base = at // BLK * BLK
        t0 = at - base
        for block in range(t0 // rows, (t0 + piece - 1) // rows + 1):
            if not kind:
                need_weights(block)
        for other in range(base // piece, gp + 1):
            need(other, kind)
        weights = wguest if kind else wbuf
        keep = (
            lax.broadcasted_iota(jnp.int32, (piece, piece), 1)
            <= lax.broadcasted_iota(jnp.int32, (piece, piece), 0)
        )
        lo, mid = base + kind * tail, at + kind * tail
        for g in range(groups):
            lanes = slice(g * GD, (g + 1) * GD)
            diag = weights[g, t0:t0 + piece, t0:t0 + piece]
            diag = jnp.where(keep, diag, jnp.zeros_like(diag))
            acc = jnp.dot(diag, ex[mid:mid + piece, lanes], preferred_element_type=jnp.float32)
            if t0:
                acc += jnp.dot(
                    weights[g, t0:t0 + piece, :t0], ex[lo:mid, lanes],
                    preferred_element_type=jnp.float32,
                )
            acc += bcol[kind, t0:t0 + piece, g:g + 1]
            rsend[mid:mid + piece, lanes] = acc.astype(jnp.bfloat16)
        dest = gp // pieces

        @pl.when(z == dest)
        def _():
            back_own(gp, z - half * kind, kind, gp % pieces).start()

        @pl.when(z != dest)
        def _():
            back(gp, z - half * kind, kind, dest).start()

    if tail:
        first_late = BLK // piece

        @pl.when(upper == 1)
        def _():
            for gp in range(first_late, total):
                mix(gp, 0)

        late_blocks = sorted(weights_in)
        weights_in.clear()

        @pl.when(upper == 0)
        def _():
            for block in late_blocks:
                need_weights(block)

        mix(0, 0)
        mix(1, 0)

        @pl.when(xi == 0)
        def _():
            rest_of_weights()

        @pl.when(upper == 1)
        def _():
            pairs = groups // 2
            near = [2 * k + xi for k in range(pairs)]
            far = [2 * k + 1 - xi for k in range(pairs)]
            for g in near:
                gz(g, z).wait_recv()
                gx(g).start()
                gy(g, p).start()
                gc(g, p, core).start()
            for g in far:
                gx(g).wait_recv()
                gy(g, p).start()
                gc(g, p, core).start()
            for g in near + far:
                gy(g, 1 - p).wait_recv()
                gc(g, 1 - p, core).start()

        mix(2, 0)

        @pl.when(upper == 1)
        def _():
            for g in range(groups):
                for q in range(ngrp):
                    gc(g, q, 1 - core).wait_recv()
            bias_up(z).wait_recv()
            bcol[1] = gbias[...].T
            for gp in range(first_late, total):
                mix(gp, 1)

        for gp in range(3, first_late):
            mix(gp, 0)
    else:
        for gp in range(total):
            mix(gp, 0)

    def gate_out(i, c):
        lanes = pl.ds(pl.multiple_of(c * cw, GD), cw)

        def step(s, carry):
            at = pl.ds(pl.multiple_of(i * piece + s * 16, 16), 16)
            out_ref[0, at, lanes] = (
                ggelu[at, lanes] * ret[c, at, :].astype(jnp.float32)
            ).astype(jnp.bfloat16)
            return carry

        lax.fori_loop(0, piece // 16, step, 0, unroll=2)

    for i in range(pieces):
        for j in reversed(range(nsp)):
            c = peer_at(j)
            gp = z * pieces + i
            kind = kind_of(gp, c)

            @pl.when(c + half * kind == z)
            def _(gp=gp, c=c, kind=kind, i=i):
                back_own(gp, c, kind, i).wait()

            @pl.when(c + half * kind != z)
            def _(c=c, i=i):
                back(i, c, 0, c).wait_recv()

            gate_out(i, c)

    for i in range(pieces):
        each_chunk(i, lambda i, c, kind: forward(i, c, z, kind).wait_send(), None)

    def back_sent(gp, kind):
        @pl.when(z != gp // pieces)
        def _():
            back(gp, z - half * kind, kind, gp // pieces).wait_send()

    early = BLK // piece if tail else total
    for gp in range(early):
        back_sent(gp, 0)
    if tail:
        @pl.when(upper == 1)
        def _():
            for gp in range(early, total):
                back_sent(gp, 0)
                back_sent(gp, 1)
            for g in range(groups):
                gy(g, p).wait_send()
                for q in range(ngrp):
                    gc(g, q, core).wait_send()
            for k in range(groups // 2):
                gx(2 * k + xi).wait_send()

        @pl.when(upper == 0)
        def _():
            for k in range(groups // 2):
                gz(2 * k + xi, z + half).wait_send()
            bias_up(z + half).wait_send()

    halves(xi, lambda h: w_own(h).wait_send())
    for g in range(groups):
        for k in range(1, nx):
            halves(xi, lambda h: w_x(g, xi, lax.rem(xi + k, nx), k - 1, h).wait_send())
            src = lax.rem(xi + k, nx)

            def sent(h):
                for m in range(1, ngrp):
                    w_y(g, src, p, m - 1, lax.rem(p + m, ngrp), h).wait_send()
                for q in range(ngrp):
                    w_c(g, src, q, core, h).wait_send()

            halves(src, sent)


def v_piece(span):
    return 128 if span % 128 == 0 else span


def body(ngrp, nsp, ndp, gate_input, value_input, norm_gain, norm_bias, mix_weight, mix_bias):
    _, span, width = value_input.shape
    groups = mix_weight.shape[0]
    cw = groups * GD
    pieces = span // v_piece(span)
    nx = ndp // 2
    total = nsp * pieces
    tail = guest_rows(ngrp, nsp, ndp, span)
    kinds, guest = (2, tail) if tail else (1, 16)
    bias = jnp.pad(mix_bias.astype(jnp.float32), ((0, -groups % 8), (0, 0)))
    dma = pltpu.SemaphoreType.DMA
    bf16, f32 = jnp.bfloat16, jnp.float32
    vmem, hbm = pl.BlockSpec(memory_space=pltpu.VMEM), pl.BlockSpec(memory_space=pl.ANY)
    return pl.pallas_call(
        functools.partial(kernel, ngrp, nsp, ndp),
        out_shape=jax.ShapeDtypeStruct(value_input.shape, bf16),
        in_specs=[hbm, hbm, vmem, vmem, hbm, vmem],
        out_specs=vmem,
        scratch_shapes=[
            pltpu.VMEM((span, width), bf16),
            pltpu.VMEM((span, width), bf16),
            pltpu.VMEM((span, width), f32),
            pltpu.VMEM((nsp, span, cw), bf16),
            pltpu.VMEM((nsp * span + tail, cw), bf16),
            pltpu.VMEM((nsp * span + tail, cw), bf16),
            pltpu.VMEM((nsp, span, cw), bf16),
            pltpu.VMEM((groups, BLK, BLK), bf16),
            pltpu.VMEM((groups, guest, guest), bf16),
            pltpu.VMEM(bias.shape, f32),
            pltpu.VMEM((kinds, BLK, bias.shape[0]), f32),
            dma((pieces,)), dma, dma, dma((kinds, pieces)), dma((kinds, pieces)),
            dma((pieces, nsp)), dma((kinds, pieces, nsp)),
            dma((kinds, total)), dma((nsp, pieces)),
            dma((2,)), dma((2,)),
            dma((max(nx - 1, 1), groups, 2)), dma((nx, groups, 2)),
            dma((max(ngrp - 1, 1), nx, groups, 2)), dma((ngrp, nx, groups, 2)),
            dma((ngrp, nx, groups, 2)), dma((ngrp, nx, groups, 2)),
            dma((groups,)), dma((groups,)), dma((groups,)), dma((groups,)),
            dma((groups,)), dma((groups,)), dma((ngrp, groups)), dma((ngrp, groups)), dma, dma,
        ],
        compiler_params=pltpu.CompilerParams(
            collective_id=0, has_side_effects=True, vmem_limit_bytes=62 * 1024 * 1024
        ),
    )(
        value_input, gate_input, norm_gain[None], norm_bias[None], mix_weight,
        bias,
    )


def solution(mesh):
    placed = (
        P(("grp", "dp"), "sp", None),
        P(("grp", "dp"), "sp", None),
        P(),
        P(),
        P("sp", "dp", None),
        P("sp", None),
    )
    return jax.shard_map(
        functools.partial(body, mesh.shape["grp"], mesh.shape["sp"], mesh.shape["dp"]),
        mesh=mesh, in_specs=placed, out_specs=P(("grp", "dp"), "sp", None), check_vma=False,
    )
```
